32 devices in a mesh: fs: 16 (over z, y, x), tp: 2 (over core).
Axes of the slice: x: 2, y: 2, z: 4, core: 2. Of those that a mesh axis runs over, the one named last changes fastest.
Arguments:
- tokens: bfloat16 [12288, 2048], P('fs'), may hold values from -6 to 6
- norm_gain: float32 [2048], replicated, may hold values from 0.1 to 1.9
- gate_weight: bfloat16 [2048, 5120], P('fs', 'tp'), may hold values from -0.125 to 0.125
- up_weight: bfloat16 [2048, 5120], P('fs', 'tp'), may hold values from -0.125 to 0.125
- down_weight: bfloat16 [5120, 2048], P('tp', 'fs'), may hold values from -0.078125 to 0.078125
Outputs:
- mixed: bfloat16 [12288, 2048], P(('fs', 'tp'))
The draws below stay inside these ranges and needn't reach their ends.
All inputs are finite; a program needn't handle non-finite values.
Results may differ from the reference program's by a relative error of at most 0.014.
Values may be sent and summed in bfloat16 or wider, within the bound.
A program may use at most 128 MiB of HBM per device.

```python
import jax
import jax.numpy as jnp
from jax import lax

D = 2048
FF = 5120
TOKENS = 12288
N_TP = 2


def levels(stream_key, dims, split, low, largest):
    level, own = 1.0, jax.random.fold_in(stream_key, 6)
    for dim, parts in split:
        steps = jnp.exp(jax.random.uniform(jax.random.fold_in(own, dim), (parts,), jnp.float32, low / len(split), largest / len(split)))
        level = level * jnp.repeat(steps, dims[dim] // parts).reshape([-1 if axis == dim else 1 for axis in range(len(dims))])
    return level


def noise(rng, shape, spread, bound, pieces=(), dtype=jnp.bfloat16):
    result = spread * jax.random.normal(rng, shape, jnp.float32)
    if pieces:
        result = result * levels(rng, shape, pieces, -0.22, 0.18)
    return jnp.clip(result, -bound, bound).astype(dtype)


def setup_inputs(seed: int = 0) -> dict:
    splits = jax.random.split(jax.random.key(seed), 6)
    tokens = noise(splits[0], (TOKENS, D), 1.0, 6.0, ((0, 16),))
    norm_gain = jnp.clip(1.0 + 0.18 * jax.random.normal(splits[1], (D,), jnp.float32), 0.1, 1.9)
    gate_weight = noise(splits[2], (D, FF), D ** -0.5, 0.125, ((0, 16), (1, 2)))
    up_weight = noise(splits[3], (D, FF), D ** -0.5, 0.125, ((0, 16), (1, 2)))
    down_weight = noise(splits[4], (FF, D), FF ** -0.5, 0.078125, ((0, 2), (1, 16)))
    return dict(tokens=tokens, norm_gain=norm_gain, gate_weight=gate_weight, up_weight=up_weight, down_weight=down_weight)


def reference(tokens, norm_gain, gate_weight, up_weight, down_weight):
    values = tokens.astype(jnp.float32)
    scale = lax.rsqrt(lax.optimization_barrier(jnp.mean(values * values, axis=-1, keepdims=True)) + 1e-06)
    normed = (values * scale * norm_gain).astype(jnp.bfloat16)
    gate_proj = jnp.dot(normed, gate_weight, preferred_element_type=jnp.float32)
    up_proj = jnp.dot(normed, up_weight, preferred_element_type=jnp.float32)
    hidden = (jax.nn.silu(gate_proj) * up_proj).astype(jnp.bfloat16)
    block = FF // N_TP
    total = jnp.zeros((tokens.shape[0], D), jnp.float32)
    for index in range(N_TP):
        part_sum = jnp.dot(hidden[:, index * block:(index + 1) * block], down_weight[index * block:(index + 1) * block, :], preferred_element_type=jnp.float32).astype(jnp.bfloat16)
        total = total + part_sum.astype(jnp.float32)
    return total.astype(jnp.bfloat16)
```

```python
import functools

import jax
import jax.numpy as jnp
from jax import lax
from jax.experimental import pallas as pl
from jax.experimental.pallas import tpu as pltpu
from jax.sharding import PartitionSpec as P

MESH = pl.DeviceIdType.MESH
PLANE = 4
ORDER = ((1, 1), (0, 1), (1, 0), (0, 0))


def simple(tokens, norm_gain, gate_weight, up_weight, down_weight):
    values = tokens.astype(jnp.float32)
    scale = lax.rsqrt(jnp.mean(values * values, axis=-1, keepdims=True) + 1e-06)
    normed = (values * scale * norm_gain).astype(jnp.bfloat16)

    def project(piece):
        whole = lax.all_gather(piece, "fs", axis=0, tiled=True)
        return jnp.dot(normed, whole, preferred_element_type=jnp.float32)

    hidden = (jax.nn.silu(project(gate_weight)) * project(up_weight)).astype(jnp.bfloat16)
    down_whole = lax.all_gather(down_weight, "fs", axis=1, tiled=True)
    return lax.psum_scatter(
        jnp.dot(hidden, down_whole, preferred_element_type=jnp.float32).astype(jnp.bfloat16),
        "tp",
        scatter_dimension=0,
        tiled=True,
    )


def kernel(nz, tok_hbm, gain_ref, gate_hbm, up_hbm, down_hbm, out_ref,
           tok, normed, gu, dn, hidden, psend, precv, own,
           loc_sem, a2a_s, a2a_r, tok_s, tok_r, up_s, dn_s, z_r, sib_s, sib_r, rs_s, rs_r):
    f = lax.axis_index("fs")
    c = lax.axis_index("tp")
    z, p = f // PLANE, f % PLANE
    y, x = p // 2, p % 2
    depth = gate_hbm.shape[0]
    width = gate_hbm.shape[1] // PLANE
    rows = tok_hbm.shape[0] // 2
    unit = depth * PLANE

    def member(k):
        oy, ox = ORDER[k]
        return ((y + oy) % 2) * 2 + (x + ox) % 2

    def dev(plane, z_, core):
        return (z_ * PLANE + plane, core)

    barrier = pltpu.get_barrier_semaphore()
    for k in range(3):
        pl.semaphore_signal(barrier, inc=1, device_id=dev(member(k), z, c), device_id_type=MESH)
    pl.semaphore_signal(barrier, inc=1, device_id=(f, 1 - c), device_id_type=MESH)

    @pl.when(z > 0)
    def _():
        pl.semaphore_signal(barrier, inc=1, device_id=dev(p, z - 1, c), device_id_type=MESH)

    @pl.when(z < nz - 1)
    def _():
        pl.semaphore_signal(barrier, inc=1, device_id=dev(p, z + 1, c), device_id_type=MESH)

    pl.semaphore_wait(barrier, 4 + (z + nz - 1) // nz + (2 * nz - 2 - z) // nz)

    sources = (gate_hbm, up_hbm, down_hbm)

    def piece_src(m, q):
        start = pl.multiple_of(q * width, 128)
        if m < 2:
            return sources[m].at[:, pl.ds(start, width)]
        return sources[m].at[pl.ds(start, width), :]

    def weight_dst(m, start, size):
        start = pl.multiple_of(start, 128)
        units = pl.ds(pl.multiple_of(c * width, 128), width)
        if m < 2:
            return gu.at[m, pl.ds(start, size), units]
        return dn.at[units, pl.ds(start, size)]

    def weight_sib(m, start, size):
        start = pl.multiple_of(start, 128)
        units = pl.ds(pl.multiple_of((1 - c) * width, 128), width)
        if m < 2:
            return gu.at[m, pl.ds(start, size), units]
        return dn.at[units, pl.ds(start, size)]

    def a2a(m, k):
        q = member(k)
        return pltpu.make_async_remote_copy(
            src_ref=piece_src(m, q), dst_ref=weight_dst(m, f * depth, depth),
            send_sem=a2a_s.at[m, k], recv_sem=a2a_r.at[m, k],
            device_id=dev(q, z, c), device_id_type=MESH)

    def a2a_in(m, k):
        q = member(k)
        ref = weight_dst(m, (z * PLANE + q) * depth, depth)
        return pltpu.make_async_remote_copy(
            src_ref=ref, dst_ref=ref, send_sem=a2a_s.at[m, k], recv_sem=a2a_r.at[m, k],
            device_id=dev(q, z, c), device_id_type=MESH)

    def local(m):
        return pltpu.make_async_copy(piece_src(m, p), weight_dst(m, f * depth, depth), loc_sem.at[m])

    half = pl.ds(pl.multiple_of(c * rows, 16), rows)

    def tok_copy(k):
        q = member(k)
        return pltpu.make_async_remote_copy(
            src_ref=tok_hbm.at[half, :], dst_ref=tok.at[k],
            send_sem=tok_s.at[k], recv_sem=tok_r.at[k],
            device_id=dev(q, z, c), device_id_type=MESH)

    own_tok = pltpu.make_async_copy(tok_hbm.at[half, :], tok.at[3], loc_sem.at[3])

    def along(m, zs, step):
        ref = weight_dst(m, zs * unit, unit)
        sems = up_s if step > 0 else dn_s
        return pltpu.make_async_remote_copy(
            src_ref=ref, dst_ref=ref, send_sem=sems.at[m, zs], recv_sem=z_r.at[m, zs],
            device_id=dev(p, z + step, c), device_id_type=MESH)

    def to_sibling(m, zs):
        ref = weight_dst(m, zs * unit, unit)
        return pltpu.make_async_remote_copy(
            src_ref=ref, dst_ref=ref, send_sem=sib_s.at[m, zs], recv_sem=sib_r.at[m, zs],
            device_id=(f, 1 - c), device_id_type=MESH)

    def from_sibling(m, zs):
        ref = weight_sib(m, zs * unit, unit)
        return pltpu.make_async_remote_copy(
            src_ref=ref, dst_ref=ref, send_sem=sib_s.at[m, zs], recv_sem=sib_r.at[m, zs],
            device_id=(f, 1 - c), device_id_type=MESH)

    def forward(m, zs):
        @pl.when((zs <= z) & (z < nz - 1))
        def _():
            along(m, zs, 1).start()

        @pl.when((zs >= z) & (z > 0))
        def _():
            along(m, zs, -1).start()

        to_sibling(m, zs).start()

    def arrived(m, zs):
        along(m, zs, 1).wait_recv()

    for m in range(3):
        for k in range(3):
            a2a(m, k).start()
        local(m).start()
    for k in range(3):
        tok_copy(k).start()
    own_tok.start()

    def own_unit(m):
        local(m).wait()
        for k in range(3):
            a2a_in(m, k).wait_recv()
        forward(m, z)

    own_unit(0)
    own_unit(1)
    for d in range(1, nz):
        for m in range(2):
            @pl.when(z - d >= 0)
            def _():
                arrived(m, z - d)
                forward(m, z - d)

            @pl.when(z + d < nz)
            def _():
                arrived(m, z + d)
                forward(m, z + d)
    own_unit(2)
    inner = (z > 0) & (z < nz - 1)
    for d in range(1, nz):
        @pl.when(inner & (z - d >= 0))
        def _():
            arrived(2, z - d)
            forward(2, z - d)

        @pl.when(inner & (z + d < nz))
        def _():
            arrived(2, z + d)
            forward(2, z + d)

    for m in range(2):
        for zs in range(nz):
            from_sibling(m, zs).wait_recv()

    def make_hidden(k):
        if k == 3:
            own_tok.wait()
        else:
            tok_copy(k).wait_recv()
        block = rows // 6

        @pl.loop(0, 6)
        def _(i):
            at = pl.ds(pl.multiple_of(i * block, 16), block)
            values = tok[k, at, :].astype(jnp.float32)
            scale = lax.rsqrt(jnp.mean(values * values, axis=-1, keepdims=True) + 1e-06)
            normed[at, :] = (values * scale * gain_ref[...]).astype(jnp.bfloat16)

        @pl.loop(0, 2 * width // 256)
        def _(j):
            at = pl.ds(pl.multiple_of(j * 256, 256), 256)
            gate = jnp.dot(normed[...], gu[0, :, at], preferred_element_type=jnp.float32)
            up = jnp.dot(normed[...], gu[1, :, at], preferred_element_type=jnp.float32)
            hidden[k, :, at] = (gate / (1.0 + jnp.exp(-gate)) * up).astype(jnp.bfloat16)

    def rs_copy(k, step, columns):
        return pltpu.make_async_remote_copy(
            src_ref=psend.at[k, :, columns], dst_ref=precv.at[k, :, columns],
            send_sem=rs_s.at[k, step], recv_sem=rs_r.at[k, step],
            device_id=dev(member(k), z, c), device_id_type=MESH)

    def plane_at(step):
        return (z + step * (1 - 2 * (z // (nz // 2))) + nz) % nz

    def columns_at(step):
        return pl.ds(pl.multiple_of(plane_at(step) * unit, 128), unit)

    for step in range(nz):
        zs = plane_at(step)
        if step > 0:
            @pl.when(jnp.logical_not(inner))
            def _():
                arrived(2, zs)
                to_sibling(2, zs).start()
        from_sibling(2, zs).wait_recv()
        columns = columns_at(step)
        for k in range(PLANE):
            if step == 0:
                make_hidden(k)

            @pl.loop(0, unit // 256)
            def _(j):
                at = pl.ds(pl.multiple_of(zs * unit + j * 256, 256), 256)
                part = jnp.dot(hidden[k], dn[:, at], preferred_element_type=jnp.float32)
                if k == 3:
                    own[:, at] = part
                else:
                    psend[k, :, at] = part.astype(jnp.bfloat16)

            if k < 3:
                rs_copy(k, step, columns).start()

    for step in range(nz):
        columns = columns_at(step)
        for k in range(3):
            rs_copy(k, step, columns).wait_recv()

        @pl.loop(0, unit // 256)
        def _(j):
            at = pl.ds(pl.multiple_of(plane_at(step) * unit + j * 256, 256), 256)
            total = own[:, at]
            for k in range(3):
                total = total + precv[k, :, at].astype(jnp.float32)
            out_ref[:, at] = total.astype(out_ref.dtype)

    for m in range(3):
        for k in range(3):
            a2a(m, k).wait_send()
        for zs in range(nz):
            to_sibling(m, zs).wait_send()

            @pl.when((zs <= z) & (z < nz - 1))
            def _():
                along(m, zs, 1).wait_send()

            @pl.when((zs >= z) & (z > 0))
            def _():
                along(m, zs, -1).wait_send()
    for k in range(3):
        tok_copy(k).wait_send()
        for step in range(nz):
            rs_copy(k, step, columns_at(step)).wait_send()


def fused(nfs, tokens, norm_gain, gate_weight, up_weight, down_weight):
    nz = nfs // PLANE
    features = tokens.shape[1]
    rows = tokens.shape[0] // 2
    width = gate_weight.shape[1] // PLANE
    any_spec = pl.BlockSpec(memory_space=pl.ANY)
    vmem_spec = pl.BlockSpec(memory_space=pltpu.VMEM)
    dma = pltpu.SemaphoreType.DMA
    bf16 = jnp.bfloat16
    return pl.pallas_call(
        functools.partial(kernel, nz),
        out_shape=jax.ShapeDtypeStruct((rows, features), bf16),
        in_specs=[any_spec, vmem_spec, any_spec, any_spec, any_spec],
        out_specs=vmem_spec,
        scratch_shapes=[
            pltpu.VMEM((PLANE, rows, features), bf16),
            pltpu.VMEM((rows, features), bf16),
            pltpu.VMEM((2, features, 2 * width), bf16),
            pltpu.VMEM((2 * width, features), bf16),
            pltpu.VMEM((PLANE, rows, 2 * width), bf16),
            pltpu.VMEM((3, rows, features), bf16),
            pltpu.VMEM((3, rows, features), bf16),
            pltpu.VMEM((rows, features), jnp.float32),
            dma((4,)), dma((3, 3)), dma((3, 3)), dma((3,)), dma((3,)),
            dma((3, nz)), dma((3, nz)), dma((3, nz)), dma((3, nz)), dma((3, nz)),
            dma((3, nz)), dma((3, nz)),
        ],
        compiler_params=pltpu.CompilerParams(
            collective_id=0, has_side_effects=True, vmem_limit_bytes=60 * 1024 * 1024
        ),
    )(tokens, norm_gain.reshape(1, features), gate_weight, up_weight, down_weight)


def per_device(nfs, ntp, tokens, norm_gain, gate_weight, up_weight, down_weight):
    rows, depth = tokens.shape[0] // 2, gate_weight.shape[0]
    fits = (
        ntp == 2
        and nfs % PLANE == 0
        and (nfs // PLANE) % 2 == 0
        and rows % 96 == 0
        and depth % 128 == 0
        and depth * nfs == tokens.shape[1]
        and gate_weight.shape[1] % (PLANE * 128) == 0
    )
    body = functools.partial(fused, nfs) if fits else simple
    return body(tokens, norm_gain, gate_weight, up_weight, down_weight)


def solution(mesh):
    in_specs = (P("fs", None), P(), P("fs", "tp"), P("fs", "tp"), P("tp", "fs"))
    out_specs = P(("fs", "tp"), None)
    body = functools.partial(per_device, mesh.shape["fs"], mesh.shape["tp"])
    return jax.shard_map(
        body, mesh=mesh, in_specs=in_specs, out_specs=out_specs, check_vma=False
    )
```

```python
import functools

import jax
import jax.numpy as jnp
from jax import lax
from jax.experimental import pallas as pl
from jax.experimental.pallas import tpu as pltpu
from jax.sharding import PartitionSpec as P

MESH = pl.DeviceIdType.MESH
PLANE = 4
ORDER = ((1, 1), (0, 1), (1, 0), (0, 0))


def simple(tokens, norm_gain, gate_weight, up_weight, down_weight):
    values = tokens.astype(jnp.float32)
    scale = lax.rsqrt(jnp.mean(values * values, axis=-1, keepdims=True) + 1e-06)
    normed = (values * scale * norm_gain).astype(jnp.bfloat16)

    def project(piece):
        whole = lax.all_gather(piece, "fs", axis=0, tiled=True)
        return jnp.dot(normed, whole, preferred_element_type=jnp.float32)

    hidden = (jax.nn.silu(project(gate_weight)) * project(up_weight)).astype(jnp.bfloat16)
    down_whole = lax.all_gather(down_weight, "fs", axis=1, tiled=True)
    return lax.psum_scatter(
        jnp.dot(hidden, down_whole, preferred_element_type=jnp.float32).astype(jnp.bfloat16),
        "tp",
        scatter_dimension=0,
        tiled=True,
    )


def kernel(nz, tok_hbm, gain_ref, gate_hbm, up_hbm, down_hbm, out_ref,
           tok, normed, gu, dn, hidden, psend, precv, own,
           loc_sem, a2a_s, a2a_r, tok_s, tok_r, up_s, dn_s, z_r, sib_s, sib_r, one_s, one_r, rs_s, rs_r):
    f = lax.axis_index("fs")
    c = lax.axis_index("tp")
    z, p = f // PLANE, f % PLANE
    y, x = p // 2, p % 2
    depth = gate_hbm.shape[0]
    width = gate_hbm.shape[1] // PLANE
    rows = tok_hbm.shape[0] // 2
    unit = depth * PLANE

    def member(k):
        oy, ox = ORDER[k]
        return ((y + oy) % 2) * 2 + (x + ox) % 2

    def dev(plane, z_, core):
        return (z_ * PLANE + plane, core)

    barrier = pltpu.get_barrier_semaphore()
    for k in range(3):
        pl.semaphore_signal(barrier, inc=1, device_id=dev(member(k), z, c), device_id_type=MESH)
    pl.semaphore_signal(barrier, inc=1, device_id=(f, 1 - c), device_id_type=MESH)

    @pl.when(z > 0)
    def _():
        pl.semaphore_signal(barrier, inc=1, device_id=dev(p, z - 1, c), device_id_type=MESH)

    @pl.when(z < nz - 1)
    def _():
        pl.semaphore_signal(barrier, inc=1, device_id=dev(p, z + 1, c), device_id_type=MESH)

    pl.semaphore_wait(barrier, 4 + (z + nz - 1) // nz + (2 * nz - 2 - z) // nz)

    sources = (gate_hbm, up_hbm, down_hbm)

    def piece_src(m, q):
        start = pl.multiple_of(q * width, 128)
        if m < 2:
            return sources[m].at[:, pl.ds(start, width)]
        return sources[m].at[pl.ds(start, width), :]

    def weight_dst(m, start, size):
        start = pl.multiple_of(start, 128)
        units = pl.ds(pl.multiple_of(c * width, 128), width)
        if m < 2:
            return gu.at[m, pl.ds(start, size), units]
        return dn.at[units, pl.ds(start, size)]

    def weight_sib(m, start, size):
        start = pl.multiple_of(start, 128)
        units = pl.ds(pl.multiple_of((1 - c) * width, 128), width)
        if m < 2:
            return gu.at[m, pl.ds(start, size), units]
        return dn.at[units, pl.ds(start, size)]

    def a2a(m, k):
        q = member(k)
        return pltpu.make_async_remote_copy(
            src_ref=piece_src(m, q), dst_ref=weight_dst(m, f * depth, depth),
            send_sem=a2a_s.at[m, k], recv_sem=a2a_r.at[m, k],
            device_id=dev(q, z, c), device_id_type=MESH)

    def a2a_in(m, k):
        q = member(k)
        ref = weight_dst(m, (z * PLANE + q) * depth, depth)
        return pltpu.make_async_remote_copy(
            src_ref=ref, dst_ref=ref, send_sem=a2a_s.at[m, k], recv_sem=a2a_r.at[m, k],
            device_id=dev(q, z, c), device_id_type=MESH)

    def local(m):
        return pltpu.make_async_copy(piece_src(m, p), weight_dst(m, f * depth, depth), loc_sem.at[m])

    half = pl.ds(pl.multiple_of(c * rows, 16), rows)

    def tok_copy(k):
        q = member(k)
        return pltpu.make_async_remote_copy(
            src_ref=tok_hbm.at[half, :], dst_ref=tok.at[k],
            send_sem=tok_s.at[k], recv_sem=tok_r.at[k],
            device_id=dev(q, z, c), device_id_type=MESH)

    own_tok = pltpu.make_async_copy(tok_hbm.at[half, :], tok.at[3], loc_sem.at[3])

    def along(m, zs, step):
        ref = weight_dst(m, zs * unit, unit)
        sems = up_s if step > 0 else dn_s
        return pltpu.make_async_remote_copy(
            src_ref=ref, dst_ref=ref, send_sem=sems.at[m, zs], recv_sem=z_r.at[m, zs],
            device_id=dev(p, z + step, c), device_id_type=MESH)

    def to_sibling(m, zs):
        ref = weight_dst(m, zs * unit, unit)
        return pltpu.make_async_remote_copy(
            src_ref=ref, dst_ref=ref, send_sem=sib_s.at[m, zs], recv_sem=sib_r.at[m, zs],
            device_id=(f, 1 - c), device_id_type=MESH)

    def from_sibling(m, zs):
        ref = weight_sib(m, zs * unit, unit)
        return pltpu.make_async_remote_copy(
            src_ref=ref, dst_ref=ref, send_sem=sib_s.at[m, zs], recv_sem=sib_r.at[m, zs],
            device_id=(f, 1 - c), device_id_type=MESH)

    def forward(m, zs):
        @pl.when((zs <= z) & (z < nz - 1))
        def _():
            along(m, zs, 1).start()

        @pl.when((zs >= z) & (z > 0))
        def _():
            along(m, zs, -1).start()

        to_sibling(m, zs).start()

    def arrived(m, zs):
        along(m, zs, 1).wait_recv()

    def piece(m, k, step):
        ref = weight_dst(m, (z * PLANE + member(k)) * depth, depth)
        sems = up_s if step > 0 else dn_s
        return pltpu.make_async_remote_copy(
            src_ref=piece_src(m, p) if k == 3 else ref, dst_ref=ref,
            send_sem=sems.at[m, z], recv_sem=z_r.at[m, z],
            device_id=dev(p, z + step, c), device_id_type=MESH)

    def pass_piece(m, k):
        @pl.when(z < nz - 1)
        def _():
            piece(m, k, 1).start()

        @pl.when(z > 0)
        def _():
            piece(m, k, -1).start()

    for m in range(3):
        for k in (1, 2, 0):
            a2a(m, k).start()
        local(m).start()
        if m < 2:
            pass_piece(m, 3)
    for k in (1, 2, 0):
        tok_copy(k).start()
    own_tok.start()

    def own_unit(m):
        if m == 2:
            pass_piece(m, 3)
        for k in (1, 2, 0):
            a2a_in(m, k).wait_recv()
            pass_piece(m, k)
        local(m).wait()
        to_sibling(m, z).start()

    own_unit(0)
    own_unit(1)
    for d in range(1, nz):
        for m in range(2):
            @pl.when(z - d >= 0)
            def _():
                arrived(m, z - d)
                forward(m, z - d)

            @pl.when(z + d < nz)
            def _():
                arrived(m, z + d)
                forward(m, z + d)
    own_unit(2)
    inner = (z > 0) & (z < nz - 1)

    def relay_down(d):
        @pl.when(inner & (z - d >= 0))
        def _():
            arrived(2, z - d)
            forward(2, z - d)

        @pl.when(inner & (z + d < nz))
        def _():
            arrived(2, z + d)
            forward(2, z + d)

    for m in range(2):
        for zs in range(nz):
            from_sibling(m, zs).wait_recv()

    def make_hidden(k):
        if k == 3:
            own_tok.wait()
        else:
            tok_copy(k).wait_recv()
        block = rows // 6

        @pl.loop(0, 6)
        def _(i):
            at = pl.ds(pl.multiple_of(i * block, 16), block)
            values = tok[k, at, :].astype(jnp.float32)
            scale = lax.rsqrt(jnp.mean(values * values, axis=-1, keepdims=True) + 1e-06)
            normed[at, :] = (values * scale * gain_ref[...]).astype(jnp.bfloat16)

        @pl.loop(0, 2 * width // 256)
        def _(j):
            at = pl.ds(pl.multiple_of(j * 256, 256), 256)
            gate = jnp.dot(normed[...], gu[0, :, at], preferred_element_type=jnp.float32)
            up = jnp.dot(normed[...], gu[1, :, at], preferred_element_type=jnp.float32)
            hidden[k, :, at] = (gate / (1.0 + jnp.exp(-gate)) * up).astype(jnp.bfloat16)

    part_rows = (pl.ds(0, rows // 2), pl.ds(rows // 2, rows // 2))

    def first(h, step):
        at = (0, part_rows[h], columns_at(step))
        return pltpu.make_async_remote_copy(
            src_ref=psend.at[at], dst_ref=precv.at[at],
            send_sem=one_s.at[h, step], recv_sem=one_r.at[h, step],
            device_id=dev(member(1 + h), z, c), device_id_type=MESH)

    def last(k, h, step):
        at = (k, part_rows[h], columns_at(step))
        return pltpu.make_async_remote_copy(
            src_ref=psend.at[at], dst_ref=precv.at[at],
            send_sem=rs_s.at[2 * k + h - 2, step], recv_sem=rs_r.at[2 * k + h - 2, step],
            device_id=dev(member(k), z, c), device_id_type=MESH)

    def plane_at(step):
        return (z + step * (1 - 2 * (z // (nz // 2))) + nz) % nz

    def columns_at(step):
        return pl.ds(pl.multiple_of(plane_at(step) * unit, 128), unit)

    def add_and_send(step):
        for h in range(2):
            k = 2 - h
            first(h, step).wait_recv()
            at = (part_rows[h], columns_at(step))
            psend[(k, *at)] = (
                psend[(k, *at)].astype(jnp.float32) + precv[(0, *at)].astype(jnp.float32)
            ).astype(jnp.bfloat16)
            last(k, h, step).start()

    for step in range(nz):
        zs = plane_at(step)
        if step > 0:
            @pl.when(jnp.logical_not(inner))
            def _():
                arrived(2, zs)
                to_sibling(2, zs).start()

            relay_down(step)
        from_sibling(2, zs).wait_recv()
        for k in range(PLANE):
            if step == 0:
                make_hidden(k)

            @pl.loop(0, unit // 256)
            def _(j):
                at = pl.ds(pl.multiple_of(zs * unit + j * 256, 256), 256)
                part = jnp.dot(hidden[k], dn[:, at], preferred_element_type=jnp.float32)
                if k == 3:
                    own[:, at] = part
                else:
                    psend[k, :, at] = part.astype(jnp.bfloat16)

            if k == 0:
                first(0, step).start()
                first(1, step).start()
            elif k < 3:
                last(k, k - 1, step).start()
        if step == 0:
            add_and_send(0)
        elif step > 1:
            add_and_send(step - 1)
    add_and_send(nz - 1)

    for step in range(nz):
        for k in (1, 2):
            for h in range(2):
                last(k, h, step).wait_recv()

        @pl.loop(0, unit // 256)
        def _(j):
            at = pl.ds(pl.multiple_of(plane_at(step) * unit + j * 256, 256), 256)
            total = own[:, at]
            for k in (1, 2):
                total = total + precv[k, :, at].astype(jnp.float32)
            out_ref[:, at] = total.astype(out_ref.dtype)

    for m in range(3):
        for k in range(3):
            a2a(m, k).wait_send()
        for zs in range(nz):
            to_sibling(m, zs).wait_send()

            @pl.when((zs <= z) & (z < nz - 1))
            def _():
                along(m, zs, 1).wait_send()

            @pl.when((zs >= z) & (z > 0))
            def _():
                along(m, zs, -1).wait_send()
    for k in range(3):
        tok_copy(k).wait_send()
    for step in range(nz):
        for h in range(2):
            first(h, step).wait_send()
            for k in (1, 2):
                last(k, h, step).wait_send()


def fused(nfs, tokens, norm_gain, gate_weight, up_weight, down_weight):
    nz = nfs // PLANE
    features = tokens.shape[1]
    rows = tokens.shape[0] // 2
    width = gate_weight.shape[1] // PLANE
    any_spec = pl.BlockSpec(memory_space=pl.ANY)
    vmem_spec = pl.BlockSpec(memory_space=pltpu.VMEM)
    dma = pltpu.SemaphoreType.DMA
    bf16 = jnp.bfloat16
    return pl.pallas_call(
        functools.partial(kernel, nz),
        out_shape=jax.ShapeDtypeStruct((rows, features), bf16),
        in_specs=[any_spec, vmem_spec, any_spec, any_spec, any_spec],
        out_specs=vmem_spec,
        scratch_shapes=[
            pltpu.VMEM((PLANE, rows, features), bf16),
            pltpu.VMEM((rows, features), bf16),
            pltpu.VMEM((2, features, 2 * width), bf16),
            pltpu.VMEM((2 * width, features), bf16),
            pltpu.VMEM((PLANE, rows, 2 * width), bf16),
            pltpu.VMEM((3, rows, features), bf16),
            pltpu.VMEM((3, rows, features), bf16),
            pltpu.VMEM((rows, features), jnp.float32),
            dma((4,)), dma((3, 3)), dma((3, 3)), dma((3,)), dma((3,)),
            dma((3, nz)), dma((3, nz)), dma((3, nz)), dma((3, nz)), dma((3, nz)),
            dma((2, nz)), dma((2, nz)), dma((4, nz)), dma((4, nz)),
        ],
        compiler_params=pltpu.CompilerParams(
            collective_id=0, has_side_effects=True, vmem_limit_bytes=60 * 1024 * 1024
        ),
    )(tokens, norm_gain.reshape(1, features), gate_weight, up_weight, down_weight)


def per_device(nfs, ntp, tokens, norm_gain, gate_weight, up_weight, down_weight):
    rows, depth = tokens.shape[0] // 2, gate_weight.shape[0]
    fits = (
        ntp == 2
        and nfs % PLANE == 0
        and (nfs // PLANE) % 2 == 0
        and rows % 96 == 0
        and depth % 128 == 0
        and depth * nfs == tokens.shape[1]
        and gate_weight.shape[1] % (PLANE * 128) == 0
    )
    body = functools.partial(fused, nfs) if fits else simple
    return body(tokens, norm_gain, gate_weight, up_weight, down_weight)


def solution(mesh):
    in_specs = (P("fs", None), P(), P("fs", "tp"), P("fs", "tp"), P("tp", "fs"))
    out_specs = P(("fs", "tp"), None)
    body = functools.partial(per_device, mesh.shape["fs"], mesh.shape["tp"])
    return jax.shard_map(
        body, mesh=mesh, in_specs=in_specs, out_specs=out_specs, check_vma=False
    )
```

```python
import functools

import jax
import jax.numpy as jnp
from jax import lax
from jax.experimental import pallas as pl
from jax.experimental.pallas import tpu as pltpu
from jax.sharding import PartitionSpec as P

MESH = pl.DeviceIdType.MESH
PLANE = 4
ORDER = ((1, 1), (0, 1), (1, 0), (0, 0))


def simple(tokens, norm_gain, gate_weight, up_weight, down_weight):
    values = tokens.astype(jnp.float32)
    scale = lax.rsqrt(jnp.mean(values * values, axis=-1, keepdims=True) + 1e-06)
    normed = (values * scale * norm_gain).astype(jnp.bfloat16)

    def project(piece):
        whole = lax.all_gather(piece, "fs", axis=0, tiled=True)
        return jnp.dot(normed, whole, preferred_element_type=jnp.float32)

    hidden = (jax.nn.silu(project(gate_weight)) * project(up_weight)).astype(jnp.bfloat16)
    down_whole = lax.all_gather(down_weight, "fs", axis=1, tiled=True)
    return lax.psum_scatter(
        jnp.dot(hidden, down_whole, preferred_element_type=jnp.float32).astype(jnp.bfloat16),
        "tp",
        scatter_dimension=0,
        tiled=True,
    )


def kernel(nz, tok_hbm, gain_ref, gate_hbm, up_hbm, down_hbm, out_ref,
           tok, acc, gu, dn, hidden, psend, precv, own,
           loc_sem, a2a_s, a2a_r, tok_s, tok_r, up_s, dn_s, z_r, sib_s, sib_r, one_s, one_r, rs_s, rs_r):
    f = lax.axis_index("fs")
    c = lax.axis_index("tp")
    z, p = f // PLANE, f % PLANE
    y, x = p // 2, p % 2
    depth = gate_hbm.shape[0]
    width = gate_hbm.shape[1] // PLANE
    rows = tok_hbm.shape[0] // 2
    unit = depth * PLANE

    def member(k):
        oy, ox = ORDER[k]
        return ((y + oy) % 2) * 2 + (x + ox) % 2

    def dev(plane, z_, core):
        return (z_ * PLANE + plane, core)

    barrier = pltpu.get_barrier_semaphore()
    for k in range(3):
        pl.semaphore_signal(barrier, inc=1, device_id=dev(member(k), z, c), device_id_type=MESH)
    pl.semaphore_signal(barrier, inc=1, device_id=(f, 1 - c), device_id_type=MESH)

    @pl.when(z > 0)
    def _():
        pl.semaphore_signal(barrier, inc=1, device_id=dev(p, z - 1, c), device_id_type=MESH)

    @pl.when(z < nz - 1)
    def _():
        pl.semaphore_signal(barrier, inc=1, device_id=dev(p, z + 1, c), device_id_type=MESH)

    pl.semaphore_wait(barrier, 4 + (z + nz - 1) // nz + (2 * nz - 2 - z) // nz)

    sources = (gate_hbm, up_hbm, down_hbm)

    def piece_src(m, q):
        start = pl.multiple_of(q * width, 128)
        if m < 2:
            return sources[m].at[:, pl.ds(start, width)]
        return sources[m].at[pl.ds(start, width), :]

    def weight_dst(m, start, size):
        start = pl.multiple_of(start, 128)
        units = pl.ds(pl.multiple_of(c * width, 128), width)
        if m < 2:
            return gu.at[m, pl.ds(start, size), units]
        return dn.at[units, pl.ds(start, size)]

    def weight_sib(m, start, size):
        start = pl.multiple_of(start, 128)
        units = pl.ds(pl.multiple_of((1 - c) * width, 128), width)
        if m < 2:
            return gu.at[m, pl.ds(start, size), units]
        return dn.at[units, pl.ds(start, size)]

    def a2a(m, k):
        q = member(k)
        return pltpu.make_async_remote_copy(
            src_ref=piece_src(m, q), dst_ref=weight_dst(m, f * depth, depth),
            send_sem=a2a_s.at[m, k], recv_sem=a2a_r.at[m, k],
            device_id=dev(q, z, c), device_id_type=MESH)

    def a2a_in(m, k):
        q = member(k)
        ref = weight_dst(m, (z * PLANE + q) * depth, depth)
        return pltpu.make_async_remote_copy(
            src_ref=ref, dst_ref=ref, send_sem=a2a_s.at[m, k], recv_sem=a2a_r.at[m, k],
            device_id=dev(q, z, c), device_id_type=MESH)

    def local(m):
        return pltpu.make_async_copy(piece_src(m, p), weight_dst(m, f * depth, depth), loc_sem.at[m])

    half = pl.ds(pl.multiple_of(c * rows, 16), rows)

    def tok_copy(k):
        q = member(k)
        return pltpu.make_async_remote_copy(
            src_ref=tok_hbm.at[half, :], dst_ref=tok.at[k],
            send_sem=tok_s.at[k], recv_sem=tok_r.at[k],
            device_id=dev(q, z, c), device_id_type=MESH)

    own_tok = pltpu.make_async_copy(tok_hbm.at[half, :], tok.at[3], loc_sem.at[3])

    def along(m, zs, step):
        ref = weight_dst(m, zs * unit, unit)
        sems = up_s if step > 0 else dn_s
        return pltpu.make_async_remote_copy(
            src_ref=ref, dst_ref=ref, send_sem=sems.at[m, zs], recv_sem=z_r.at[m, zs],
            device_id=dev(p, z + step, c), device_id_type=MESH)

    def to_sibling(m, zs):
        ref = weight_dst(m, zs * unit, unit)
        return pltpu.make_async_remote_copy(
            src_ref=ref, dst_ref=ref, send_sem=sib_s.at[m, zs], recv_sem=sib_r.at[m, zs],
            device_id=(f, 1 - c), device_id_type=MESH)

    def from_sibling(m, zs):
        ref = weight_sib(m, zs * unit, unit)
        return pltpu.make_async_remote_copy(
            src_ref=ref, dst_ref=ref, send_sem=sib_s.at[m, zs], recv_sem=sib_r.at[m, zs],
            device_id=(f, 1 - c), device_id_type=MESH)

    def forward(m, zs):
        @pl.when((zs <= z) & (z < nz - 1))
        def _():
            along(m, zs, 1).start()

        @pl.when((zs >= z) & (z > 0))
        def _():
            along(m, zs, -1).start()

        to_sibling(m, zs).start()

    def arrived(m, zs):
        along(m, zs, 1).wait_recv()

    def piece(m, k, step):
        ref = weight_dst(m, (z * PLANE + member(k)) * depth, depth)
        sems = up_s if step > 0 else dn_s
        return pltpu.make_async_remote_copy(
            src_ref=piece_src(m, p) if k == 3 else ref, dst_ref=ref,
            send_sem=sems.at[m, z], recv_sem=z_r.at[m, z],
            device_id=dev(p, z + step, c), device_id_type=MESH)

    def pass_piece(m, k):
        @pl.when(z < nz - 1)
        def _():
            piece(m, k, 1).start()

        @pl.when(z > 0)
        def _():
            piece(m, k, -1).start()

    for m in range(3):
        for k in (1, 2, 0):
            a2a(m, k).start()
        local(m).start()
        if m < 2:
            pass_piece(m, 3)
    for k in (1, 2, 0):
        tok_copy(k).start()
    own_tok.start()

    def own_unit(m):
        if m == 2:
            pass_piece(m, 3)
        for k in (1, 2, 0):
            a2a_in(m, k).wait_recv()
            pass_piece(m, k)
        local(m).wait()
        to_sibling(m, z).start()

    own_unit(0)
    own_unit(1)
    def relay_wide(d):
        for m in range(2):
            @pl.when(z - d >= 0)
            def _():
                arrived(m, z - d)
                forward(m, z - d)

            @pl.when(z + d < nz)
            def _():
                arrived(m, z + d)
                forward(m, z + d)
    for d in range(1, nz - 1):
        relay_wide(d)
    own_unit(2)
    inner = (z > 0) & (z < nz - 1)

    def relay_down(d):
        @pl.when(inner & (z - d >= 0))
        def _():
            arrived(2, z - d)
            forward(2, z - d)

        @pl.when(inner & (z + d < nz))
        def _():
            arrived(2, z + d)
            forward(2, z + d)

    end = z // (nz - 1)
    late = (nz - 1) * (1 - end)

    def project(m, k, at, start, size):
        depths = pl.ds(pl.multiple_of(start * unit, 128), size * unit)
        return jnp.dot(tok[k, :, depths], gu[m, depths, at], preferred_element_type=jnp.float32)

    for m in range(2):
        for i in range(nz - 1):
            from_sibling(m, end + i).wait_recv()
    for k in (3, 1, 2, 0):
        if k == 3:
            own_tok.wait()
        else:
            tok_copy(k).wait_recv()
        block = rows // 6

        @pl.loop(0, 6)
        def _(i):
            at = pl.ds(pl.multiple_of(i * block, 16), block)
            values = tok[k, at, :].astype(jnp.float32)
            scale = lax.rsqrt(jnp.mean(values * values, axis=-1, keepdims=True) + 1e-06)
            tok[k, at, :] = (values * scale * gain_ref[...]).astype(jnp.bfloat16)

        @pl.loop(0, 2 * width // 256)
        def _(j):
            at = pl.ds(pl.multiple_of(j * 256, 256), 256)
            for m in range(2):
                acc[m, k, :, at] = project(m, k, at, end, nz - 1)

    relay_wide(nz - 1)
    for m in range(2):
        from_sibling(m, late).wait_recv()

    def make_hidden(k):
        @pl.loop(0, 2 * width // 256)
        def _(j):
            at = pl.ds(pl.multiple_of(j * 256, 256), 256)
            gate = acc[0, k, :, at] + project(0, k, at, late, 1)
            up = acc[1, k, :, at] + project(1, k, at, late, 1)
            hidden[k, :, at] = (gate / (1.0 + jnp.exp(-gate)) * up).astype(jnp.bfloat16)

    part_rows = (pl.ds(0, rows // 2), pl.ds(rows // 2, rows // 2))

    def first(h, step):
        at = (0, part_rows[h], columns_at(step))
        return pltpu.make_async_remote_copy(
            src_ref=psend.at[at], dst_ref=precv.at[at],
            send_sem=one_s.at[h, step], recv_sem=one_r.at[h, step],
            device_id=dev(member(1 + h), z, c), device_id_type=MESH)

    def last(k, h, step):
        at = (k, part_rows[h], columns_at(step))
        return pltpu.make_async_remote_copy(
            src_ref=psend.at[at], dst_ref=precv.at[at],
            send_sem=rs_s.at[2 * k + h - 2, step], recv_sem=rs_r.at[2 * k + h - 2, step],
            device_id=dev(member(k), z, c), device_id_type=MESH)

    def plane_at(step):
        return (z + step * (1 - 2 * (z // (nz // 2))) + nz) % nz

    def columns_at(step):
        return pl.ds(pl.multiple_of(plane_at(step) * unit, 128), unit)

    def add_and_send(step):
        for h in range(2):
            k = 2 - h
            first(h, step).wait_recv()
            at = (part_rows[h], columns_at(step))
            psend[(k, *at)] = (
                psend[(k, *at)].astype(jnp.float32) + precv[(0, *at)].astype(jnp.float32)
            ).astype(jnp.bfloat16)
            last(k, h, step).start()

    for step in range(nz):
        zs = plane_at(step)
        if step > 0:
            @pl.when(jnp.logical_not(inner))
            def _():
                arrived(2, zs)
                to_sibling(2, zs).start()

            relay_down(step)
        from_sibling(2, zs).wait_recv()
        for k in range(PLANE):
            if step == 0:
                make_hidden(k)

            @pl.loop(0, unit // 256)
            def _(j):
                at = pl.ds(pl.multiple_of(zs * unit + j * 256, 256), 256)
                part = jnp.dot(hidden[k], dn[:, at], preferred_element_type=jnp.float32)
                if k == 3:
                    own[:, at] = part
                else:
                    psend[k, :, at] = part.astype(jnp.bfloat16)

            if k == 0:
                first(0, step).start()
                first(1, step).start()
            elif k < 3:
                last(k, k - 1, step).start()
        if step == 0:
            add_and_send(0)
        elif step > 1:
            add_and_send(step - 1)
    add_and_send(nz - 1)

    for step in range(nz):
        for k in (1, 2):
            for h in range(2):
                last(k, h, step).wait_recv()

        @pl.loop(0, unit // 256)
        def _(j):
            at = pl.ds(pl.multiple_of(plane_at(step) * unit + j * 256, 256), 256)
            total = own[:, at]
            for k in (1, 2):
                total = total + precv[k, :, at].astype(jnp.float32)
            out_ref[:, at] = total.astype(out_ref.dtype)

    for m in range(3):
        for k in range(3):
            a2a(m, k).wait_send()
        for zs in range(nz):
            to_sibling(m, zs).wait_send()

            @pl.when((zs <= z) & (z < nz - 1))
            def _():
                along(m, zs, 1).wait_send()

            @pl.when((zs >= z) & (z > 0))
            def _():
                along(m, zs, -1).wait_send()
    for k in range(3):
        tok_copy(k).wait_send()
    for step in range(nz):
        for h in range(2):
            first(h, step).wait_send()
            for k in (1, 2):
                last(k, h, step).wait_send()


def fused(nfs, tokens, norm_gain, gate_weight, up_weight, down_weight):
    nz = nfs // PLANE
    features = tokens.shape[1]
    rows = tokens.shape[0] // 2
    width = gate_weight.shape[1] // PLANE
    any_spec = pl.BlockSpec(memory_space=pl.ANY)
    vmem_spec = pl.BlockSpec(memory_space=pltpu.VMEM)
    dma = pltpu.SemaphoreType.DMA
    bf16 = jnp.bfloat16
    return pl.pallas_call(
        functools.partial(kernel, nz),
        out_shape=jax.ShapeDtypeStruct((rows, features), bf16),
        in_specs=[any_spec, vmem_spec, any_spec, any_spec, any_spec],
        out_specs=vmem_spec,
        scratch_shapes=[
            pltpu.VMEM((PLANE, rows, features), bf16),
            pltpu.VMEM((2, PLANE, rows, 2 * width), jnp.float32),
            pltpu.VMEM((2, features, 2 * width), bf16),
            pltpu.VMEM((2 * width, features), bf16),
            pltpu.VMEM((PLANE, rows, 2 * width), bf16),
            pltpu.VMEM((3, rows, features), bf16),
            pltpu.VMEM((3, rows, features), bf16),
            pltpu.VMEM((rows, features), jnp.float32),
            dma((4,)), dma((3, 3)), dma((3, 3)), dma((3,)), dma((3,)),
            dma((3, nz)), dma((3, nz)), dma((3, nz)), dma((3, nz)), dma((3, nz)),
            dma((2, nz)), dma((2, nz)), dma((4, nz)), dma((4, nz)),
        ],
        compiler_params=pltpu.CompilerParams(
            collective_id=0, has_side_effects=True, vmem_limit_bytes=62 * 1024 * 1024
        ),
    )(tokens, norm_gain.reshape(1, features), gate_weight, up_weight, down_weight)


def per_device(nfs, ntp, tokens, norm_gain, gate_weight, up_weight, down_weight):
    rows, depth = tokens.shape[0] // 2, gate_weight.shape[0]
    fits = (
        ntp == 2
        and nfs % PLANE == 0
        and (nfs // PLANE) % 2 == 0
        and rows % 96 == 0
        and depth % 128 == 0
        and depth * nfs == tokens.shape[1]
        and gate_weight.shape[1] % (PLANE * 128) == 0
    )
    body = functools.partial(fused, nfs) if fits else simple
    return body(tokens, norm_gain, gate_weight, up_weight, down_weight)


def solution(mesh):
    in_specs = (P("fs", None), P(), P("fs", "tp"), P("fs", "tp"), P("tp", "fs"))
    out_specs = P(("fs", "tp"), None)
    body = functools.partial(per_device, mesh.shape["fs"], mesh.shape["tp"])
    return jax.shard_map(
        body, mesh=mesh, in_specs=in_specs, out_specs=out_specs, check_vma=False
    )
```
